32 devices in a mesh: sp: 8 (over z, x), tp: 4 (over y, core).
Axes of the slice: x: 2, y: 2, z: 4, core: 2. Of those that a mesh axis runs over, the one named last changes fastest.
Arguments:
- queries: bfloat16 [3072, 768], P('sp', 'tp'), may hold values from -8 to 8
- keys: bfloat16 [3072, 256], P('sp', 'tp'), may hold values from -8 to 8
- values: bfloat16 [3072, 256], P('sp', 'tp'), may hold values from -6 to 6
- sinks: float32 [12], P('tp'), may hold values from 1 to 6
- residual: bfloat16 [3072, 2048], P('sp'), may hold values from -6 to 6
- out_weight: bfloat16 [768, 2048], replicated, may hold values from -3 to 3
- norm_gain: float32 [2048], replicated, may hold values from 0.1 to 1.9
- shared_gate: bfloat16 [2048, 512], P(None, 'tp'), may hold values from -0.125 to 0.125
- shared_up: bfloat16 [2048, 512], P(None, 'tp'), may hold values from -0.125 to 0.125
- shared_down: bfloat16 [512, 2048], P('tp'), may hold values from -0.25 to 0.25
- expert_ids: int32 [3072, 2], P('sp'), may hold values from 0 to 15, all different within a row; in each aligned block of 96 rows (0 to 95, 96 to 191, ...) at most 24 rows name the same one
- route_weights: float32 [3072, 2], P(('sp', 'tp')), may hold values from 0.2 to 2
- expert_gate: bfloat16 [16, 2048, 1024], P('sp', None, 'tp'), may hold values from -0.125 to 0.125
- expert_up: bfloat16 [16, 2048, 1024], P('sp', None, 'tp'), may hold values from -0.125 to 0.125
- expert_down: bfloat16 [16, 1024, 2048], P('sp', 'tp'), may hold values from -0.1875 to 0.1875
Outputs:
- layer_out: bfloat16 [3072, 2048], P(('sp', 'tp'))
The draws below stay inside these ranges and needn't reach their ends.
Inputs may be any that keep to these rules, and one draw needn't show every extreme that they name: `expert_ids`: each row names 2 different experts. In each aligned block of 96 rows no expert is named more than 24 times, a bound that some blocks reach.
All inputs are finite; a program needn't handle non-finite values.
Results may differ from the reference program's by a relative error of at most 0.018.
Values may be sent and summed in bfloat16 or wider, within the bound.
No kernel may reach another device: no remote copies, remote signals or barrier semaphores. Data moves between devices by JAX's collectives and lax.ppermute only.
A program may use at most 128 MiB of HBM per device.

```python
import math
import jax
import jax.numpy as jnp
import numpy as np
from jax import lax

D = 2048
HEADS = 12
KV_HEADS = 4
HEAD_DIM = 64
WINDOW = 128
GRID_W = 64
EXP_HID = 1024
SHARED_HID = 512
TOPK = 2
TOKENS = 3072
OWN = 96
EXPERTS = 16
CAP = 24
N_TP = 4


def drawn_pair(key):
    seeded = jax.random.fold_in(key, 7)
    query_seed, key_seed = jax.random.split(seeded, 2)
    queries = jnp.clip(jax.random.normal(query_seed, (TOKENS, HEADS, HEAD_DIM), jnp.float32), -6.0, 6.0)
    keys = jnp.clip(jax.random.normal(key_seed, (TOKENS, KV_HEADS, HEAD_DIM), jnp.float32), -6.0, 6.0)
    return (queries.reshape(TOKENS, HEADS * HEAD_DIM), keys.reshape(TOKENS, KV_HEADS * HEAD_DIM))


def draw_queries(key, part):
    return drawn_pair(key)[0].astype(jnp.bfloat16)


def draw_keys(key, part):
    return drawn_pair(key)[1].astype(jnp.bfloat16)


def shard_levels(own_key, dims, shards, low, largest):
    def one(position, shards_of):
        draws = jax.random.uniform(jax.random.fold_in(jax.random.fold_in(own_key, 6), position), (shards_of,), jnp.float32, low / len(shards), largest / len(shards))
        return jnp.repeat(jnp.exp(draws), dims[position] // shards_of).reshape((-1,) + (1,) * (len(dims) - position - 1))

    loudness = one(*shards[0])
    for cut in shards[1:]:
        loudness = loudness * one(*cut)
    return loudness


def assign_block(rng, own, number, rows, amount, top, bound, slope):
    sequence = jax.random.permutation(rng, amount)
    packed, usual = portions_of(amount, rows * top, bound, slope, True), portions_of(amount, rows * top, bound, slope, False)
    places = jnp.arange(amount)

    def named(tallies, turn):
        used = int((tallies > 0).sum())
        fixed = max(1, used // 4)
        moved = fixed + (places - fixed + turn * (used - fixed)) % max(1, amount - fixed)
        return jnp.zeros((amount,), jnp.int32).at[sequence[jnp.where(places < fixed, places, moved)]].set(jnp.asarray(tallies, jnp.int32))

    tallies = jnp.where(number % 4 == 0, named(packed, number // 4), named(usual, number - number // 4 - 1))
    mixed = jax.random.permutation(jax.random.fold_in(own, 3), amount)
    source_of, receiver = mixed[0:amount // 2 * 2:2], mixed[1:amount // 2 * 2:2]
    room = jnp.minimum(tallies[source_of] - 1, bound - tallies[receiver]) // 2
    room = jnp.where((source_of == sequence[0]) | (receiver == sequence[0]) | (tallies[receiver] == 0), 0, jnp.maximum(room, 0))
    moved = jax.random.randint(jax.random.fold_in(own, 4), (amount // 2,), 0, 1 << 20) % (room + 1)
    tallies = tallies.at[source_of].add(-moved).at[receiver].add(moved)
    items = jnp.searchsorted(jnp.cumsum(tallies), jnp.arange(rows * top), side="right").astype(jnp.int32)
    listing = items.reshape(top, rows).T
    listing = listing[jax.random.permutation(jax.random.fold_in(own, 1), rows)]
    turn = jax.random.randint(jax.random.fold_in(own, 2), (rows, 1), 0, top)
    return jnp.take_along_axis(listing, (jnp.arange(top)[None, :] + turn) % top, axis=1)


def portions_of(amount, total, most, slope, full):
    portions = [(1 << 20) // math.isqrt(rank ** slope) + 1 for rank in range(1, amount + 1)]
    largest = most if full else min(most, max(-(-total // amount), total * portions[0] // sum(portions)))
    least = 1 if total - largest >= amount - 1 else 0
    counts, surplus = [largest] + [least] * (amount - 1), total - largest - least * (amount - 1)
    while surplus > 0:
        free = [i for i in range(1, amount) if counts[i] < largest] or [i for i in range(1, amount) if counts[i] < most]
        pool, budget = sum([portions[i] for i in free]), surplus
        for i in free:
            more = min(most - counts[i], max(1, budget * portions[i] // pool), surplus)
            counts[i] = counts[i] + more
            surplus = surplus - more
    return np.array(counts)


def centred(rng, shape, width, limit, cuts=(), kind=jnp.bfloat16):
    gain = shard_levels(rng, shape, cuts, -0.22, 0.18) if cuts else 1.0
    values = jax.random.normal(rng, shape, jnp.float32) * width * gain
    return jnp.minimum(jnp.maximum(values, -limit), limit).astype(kind)


def setup_inputs(seed: int = 0) -> dict:
    arg_keys = jax.random.split(jax.random.key(seed), 16)
    queries = draw_queries(jax.random.fold_in(arg_keys[15], 71), 0)
    keys = draw_keys(jax.random.fold_in(arg_keys[15], 71), 0)
    values = centred(arg_keys[2], (TOKENS, KV_HEADS * HEAD_DIM), 1.0, 6.0, ((0, 8), (1, 4)))
    sinks = jnp.clip(1.0 + 5.0 * jax.random.uniform(arg_keys[3], (HEADS,), jnp.float32) ** shard_levels(arg_keys[3], (HEADS,), ((0, 4),), -0.2, 0.2), 1.0, 6.0)
    residual = centred(arg_keys[4], (TOKENS, D), 1.0, 6.0, ((0, 8),))
    out_weight = centred(arg_keys[5], (HEADS * HEAD_DIM, D), 0.5, 3.0)
    norm_gain = jnp.clip(1.0 + 0.18 * jax.random.normal(arg_keys[6], (D,), jnp.float32), 0.1, 1.9)
    shared_gate = centred(arg_keys[7], (D, SHARED_HID), D ** -0.5, 0.125, ((1, 4),))
    shared_up = centred(arg_keys[8], (D, SHARED_HID), D ** -0.5, 0.125, ((1, 4),))
    shared_down = centred(arg_keys[9], (SHARED_HID, D), SHARED_HID ** -0.5, 0.25, ((0, 4),))
    expert_ids_keys = jax.random.split(jax.random.fold_in(arg_keys[10], 1), TOKENS // OWN)
    expert_ids_turns = jax.random.permutation(jax.random.fold_in(arg_keys[10], 3), TOKENS // OWN)
    expert_ids = jax.vmap(lambda own, number: assign_block(jax.random.fold_in(arg_keys[10], 2), own, number, OWN, EXPERTS, TOPK, CAP, 2))(expert_ids_keys, expert_ids_turns).reshape((TOKENS, TOPK))
    route_weights = jnp.clip(jnp.exp(math.log(2.0) - 2.3025851 * jax.random.uniform(arg_keys[11], (TOKENS, TOPK), jnp.float32) ** shard_levels(arg_keys[11], (TOKENS, TOPK), ((0, 32),), -0.2, 0.2)), 0.2, 2.0)
    expert_gate = centred(arg_keys[12], (EXPERTS, D, EXP_HID), D ** -0.5, 0.125, ((0, 8), (2, 4)))
    expert_up = centred(arg_keys[13], (EXPERTS, D, EXP_HID), D ** -0.5, 0.125, ((0, 8), (2, 4)))
    expert_down = centred(arg_keys[14], (EXPERTS, EXP_HID, D), EXP_HID ** -0.5, 0.1875, ((0, 8), (1, 4)))
    return {"queries": queries, "keys": keys, "values": values, "sinks": sinks, "residual": residual, "out_weight": out_weight, "norm_gain": norm_gain, "shared_gate": shared_gate, "shared_up": shared_up, "shared_down": shared_down, "expert_ids": expert_ids, "route_weights": route_weights, "expert_gate": expert_gate, "expert_up": expert_up, "expert_down": expert_down}


ROPE_BASE = 10000.0
NEG_LARGE = -1e+30
NORM_EPSILON = 1e-06

def rotary_turn(values, places, turn_sign):
    halfway = values.shape[-1] // 2
    quarter = halfway // 2
    spectrum = ROPE_BASE ** (-jnp.arange(0, halfway, 2, dtype=jnp.float32) / halfway)

    def rotate_by(segment, offsets_at):
        angles = turn_sign * offsets_at.astype(jnp.float32)[:, None] * spectrum[None, :]
        cosine = jnp.cos(angles)[:, None, :]
        sine_part = jnp.sin(angles)[:, None, :]
        former = segment[..., :quarter]
        latter = segment[..., quarter:]
        return jnp.concatenate([former * cosine - latter * sine_part, former * sine_part + latter * cosine], axis=-1)
    return jnp.concatenate([rotate_by(values[..., :halfway], places // GRID_W), rotate_by(values[..., halfway:], places % GRID_W)], axis=-1)

def attend(queries, keys, values, sinks):
    group_size = HEADS // KV_HEADS
    places = jnp.arange(TOKENS, dtype=jnp.int32)
    turned_queries = rotary_turn(queries.astype(jnp.float32).reshape(TOKENS, HEADS, HEAD_DIM), places, 1.0).astype(jnp.bfloat16)
    turned_keys = rotary_turn(keys.astype(jnp.float32).reshape(TOKENS, KV_HEADS, HEAD_DIM), places, 1.0).astype(jnp.bfloat16)
    margin = ((WINDOW, WINDOW), (0, 0), (0, 0))
    padded_keys = jnp.pad(turned_keys, margin)
    padded_values = jnp.pad(values.reshape(TOKENS, KV_HEADS, HEAD_DIM), margin)
    sink_logit = sinks.astype(jnp.float32).reshape(KV_HEADS, group_size)[:, :, None, None]

    def one_block(block_index):
        start_row = block_index * WINDOW
        block_queries = lax.dynamic_slice_in_dim(turned_queries, start_row, WINDOW, 0).reshape(WINDOW, KV_HEADS, group_size, HEAD_DIM)
        block_keys = lax.dynamic_slice_in_dim(padded_keys, start_row, 3 * WINDOW, 0)
        block_values = lax.dynamic_slice_in_dim(padded_values, start_row, 3 * WINDOW, 0)
        scores = jnp.einsum('qkgd,mkd->kgqm', block_queries.astype(jnp.float32), block_keys.astype(jnp.float32)) * HEAD_DIM ** (-0.5)
        query_at = start_row + jnp.arange(WINDOW, dtype=jnp.int32)
        key_at = start_row - WINDOW + jnp.arange(3 * WINDOW, dtype=jnp.int32)
        allowed = (jnp.abs(query_at[:, None] - key_at[None, :]) <= WINDOW) & (key_at >= 0)[None, :] & (key_at < TOKENS)[None, :]
        scores = jnp.where(allowed[None, None], scores, NEG_LARGE)
        highest = jnp.maximum(lax.optimization_barrier(jnp.max(scores, axis=-1, keepdims=True)), sink_logit)
        lifted = jnp.exp(scores - highest)
        denominator = lax.optimization_barrier(jnp.sum(lifted, axis=-1, keepdims=True)) + jnp.exp(sink_logit - highest)
        probabilities = (lifted / denominator).astype(jnp.bfloat16)
        result = jnp.einsum('kgqm,mkd->qkgd', probabilities.astype(jnp.float32), block_values.astype(jnp.float32))
        return result.astype(jnp.bfloat16).reshape(WINDOW, HEADS * HEAD_DIM)
    blocks = lax.map(one_block, jnp.arange(TOKENS // WINDOW, dtype=jnp.int32))
    return blocks.reshape(TOKENS, HEADS * HEAD_DIM)

def gated_hidden(gathered_rows, gate_weight, up_weight):
    gate_values = jnp.dot(gathered_rows, gate_weight, preferred_element_type=jnp.float32)
    up_values = jnp.dot(gathered_rows, up_weight, preferred_element_type=jnp.float32)
    return (jax.nn.silu(gate_values) * up_values).astype(jnp.bfloat16)

def block_sum(hidden, down_weight):
    piece_width = hidden.shape[1] // N_TP
    running_total = jnp.zeros((hidden.shape[0], down_weight.shape[1]), jnp.float32)
    for block_index in range(N_TP):
        block_term = jnp.dot(hidden[:, block_index * piece_width:(block_index + 1) * piece_width], down_weight[block_index * piece_width:(block_index + 1) * piece_width], preferred_element_type=jnp.float32)
        running_total = running_total + lax.optimization_barrier(block_term.astype(jnp.bfloat16)).astype(jnp.float32)
    return running_total

def reference(queries, keys, values, sinks, residual, out_weight, norm_gain, shared_gate, shared_up, shared_down, expert_ids, route_weights, expert_gate, expert_up, expert_down):
    attended = attend(queries, keys, values, sinks)
    projected = jnp.dot(attended, out_weight, preferred_element_type=jnp.float32)
    mixed_rows = (residual.astype(jnp.float32) + projected).astype(jnp.bfloat16)
    mixed_float = mixed_rows.astype(jnp.float32)
    scale_rows = lax.rsqrt(lax.optimization_barrier(jnp.mean(mixed_float * mixed_float, axis=-1, keepdims=True)) + NORM_EPSILON)
    normed = (mixed_float * scale_rows * norm_gain).astype(jnp.bfloat16)
    shared_out = block_sum(gated_hidden(normed, shared_gate, shared_up), shared_down)
    owners = TOKENS // OWN
    assigns = OWN * TOPK
    route_rows = expert_ids.reshape(owners, assigns)
    order_index = jnp.arange(assigns, dtype=jnp.int32)
    earlier = order_index[None, :] < order_index[:, None]
    rank_in_block = lax.optimization_barrier(jnp.sum(((route_rows[:, :, None] == route_rows[:, None, :]) & earlier[None]).astype(jnp.int32), axis=2))
    slot_index = route_rows * CAP + rank_in_block
    owner_index = jnp.arange(owners, dtype=jnp.int32)[:, None]
    token_of = owner_index * OWN + order_index[None, :] // TOPK
    slot_token = jnp.full((owners, EXPERTS * CAP), TOKENS, jnp.int32).at[owner_index, slot_index].set(token_of)
    slot_weight = jnp.zeros((owners, EXPERTS * CAP), jnp.float32).at[owner_index, slot_index].set(route_weights.astype(jnp.float32).reshape(owners, assigns))
    normed_pad = jnp.concatenate([normed, jnp.zeros((1, D), jnp.bfloat16)], axis=0)

    def one_expert(accumulated, expert):
        tokens_here = lax.dynamic_slice_in_dim(slot_token, expert * CAP, CAP, 1).reshape(-1)
        weights_here = lax.dynamic_slice_in_dim(slot_weight, expert * CAP, CAP, 1).reshape(-1)
        gathered_rows = normed_pad[tokens_here]
        hidden = gated_hidden(gathered_rows, expert_gate[expert], expert_up[expert])
        outcome = block_sum(hidden, expert_down[expert]).astype(jnp.bfloat16)
        accumulated = accumulated.at[tokens_here].add(weights_here[:, None] * outcome.astype(jnp.float32))
        return (accumulated, None)
    accumulated, unused = lax.scan(one_expert, jnp.zeros((TOKENS + 1, D), jnp.float32), jnp.arange(EXPERTS, dtype=jnp.int32))
    return (mixed_float + shared_out + accumulated[:TOKENS]).astype(jnp.bfloat16)
```

```python
import functools

import jax
import jax.numpy as jnp
import numpy as np
from jax import lax
from jax.experimental import pallas as pl
from jax.experimental.pallas import tpu as pltpu
from jax.sharding import PartitionSpec as P

HEAD_DIM = 64
WINDOW = 128
GRID_W = 64
TOPK = 2
ROPE_BASE = 10000.0
NEG_LARGE = -1e30
NORM_EPSILON = 1e-06

BF = jnp.bfloat16
F32 = jnp.float32
VMEM_LIMIT = 56 * 1024 * 1024


def dot32(a, b):
    return jnp.dot(a, b, preferred_element_type=F32)


def call(body, outs, operands, scalars=(), scratch=(), flops=0, moved=0):
    grid_spec = pltpu.PrefetchScalarGridSpec(
        num_scalar_prefetch=len(scalars),
        grid=(),
        in_specs=[pl.BlockSpec(memory_space=pltpu.VMEM)] * len(operands),
        out_specs=[pl.BlockSpec(memory_space=pltpu.VMEM)] * len(outs),
        scratch_shapes=list(scratch),
    )
    return pl.pallas_call(
        body,
        out_shape=[jax.ShapeDtypeStruct(shape, kind) for shape, kind in outs],
        grid_spec=grid_spec,
        compiler_params=pltpu.CompilerParams(vmem_limit_bytes=VMEM_LIMIT),
        cost_estimate=pl.CostEstimate(flops=flops, bytes_accessed=moved, transcendentals=0),
    )(*scalars, *operands)


def signed_swap():
    half, quarter = HEAD_DIM // 2, HEAD_DIM // 4
    swap = np.zeros((HEAD_DIM, HEAD_DIM), np.float32)
    for base in (0, half):
        for j in range(quarter):
            swap[base + quarter + j, base + j] = -1.0
            swap[base + j, base + quarter + j] = 1.0
    return swap


def rotary_tables(places):
    half, quarter = HEAD_DIM // 2, HEAD_DIM // 4
    lane = jnp.arange(HEAD_DIM, dtype=jnp.int32)
    exponent = (2 * (lane % quarter)).astype(F32) / half
    spectrum = ROPE_BASE ** (-exponent)
    at = jnp.where(lane[None, :] < half, (places // GRID_W)[:, None], (places % GRID_W)[:, None])
    angles = at.astype(F32) * spectrum[None, :]
    return jnp.cos(angles), jnp.sin(angles)


def attention_body(
    info_ref, sink_ref, q_ref, k_ref, v_ref, before_ref, after_ref, cos_ref, sin_ref, swap_ref,
    out_ref, kx_ref, vx_ref,
):
    rows, key_width = k_ref.shape
    key_heads = key_width // HEAD_DIM
    heads = q_ref.shape[1] // HEAD_DIM
    group = heads // key_heads
    first_row, total_rows = info_ref[0], info_ref[1]
    swap = swap_ref[...]

    def turn(x, start):
        cosine = cos_ref[start : start + x.shape[0]]
        sine = sin_ref[start : start + x.shape[0]]
        return (x.astype(F32) * cosine + dot32(x, swap) * sine).astype(BF)

    for g in range(key_heads):
        cut = slice(g * HEAD_DIM, (g + 1) * HEAD_DIM)
        late = slice(key_width + g * HEAD_DIM, key_width + (g + 1) * HEAD_DIM)
        kx_ref[g, 0:WINDOW] = turn(before_ref[:, cut], 0)
        kx_ref[g, WINDOW : WINDOW + rows] = turn(k_ref[:, cut], WINDOW)
        kx_ref[g, WINDOW + rows : 2 * WINDOW + rows] = turn(after_ref[:, cut], WINDOW + rows)
        vx_ref[g, 0:WINDOW] = before_ref[:, late]
        vx_ref[g, WINDOW : WINDOW + rows] = v_ref[:, cut]
        vx_ref[g, WINDOW + rows : 2 * WINDOW + rows] = after_ref[:, late]

    query_index = lax.broadcasted_iota(jnp.int32, (WINDOW, 3 * WINDOW), 0)
    key_index = lax.broadcasted_iota(jnp.int32, (WINDOW, 3 * WINDOW), 1)
    apart = key_index - query_index
    near = (apart >= 0) & (apart <= 2 * WINDOW)
    for b in range(rows // WINDOW):
        key_at = key_index + (first_row + (b - 1) * WINDOW)
        allowed = near & (key_at >= 0) & (key_at < total_rows)
        done = []
        for h in range(heads):
            g = h // group
            q = turn(
                q_ref[b * WINDOW : (b + 1) * WINDOW, h * HEAD_DIM : (h + 1) * HEAD_DIM],
                (b + 1) * WINDOW,
            )
            keys = kx_ref[g, b * WINDOW : (b + 3) * WINDOW]
            scores = lax.dot_general(
                q, keys, (((1,), (1,)), ((), ())), preferred_element_type=F32
            ) * HEAD_DIM ** (-0.5)
            scores = jnp.where(allowed, scores, NEG_LARGE)
            sink = sink_ref[h]
            highest = jnp.maximum(jnp.max(scores, axis=1, keepdims=True), sink)
            lifted = jnp.exp(scores - highest)
            denominator = jnp.sum(lifted, axis=1, keepdims=True) + jnp.exp(sink - highest)
            probabilities = (lifted / denominator).astype(BF)
            done.append(dot32(probabilities, vx_ref[g, b * WINDOW : (b + 3) * WINDOW]).astype(BF))
        out_ref[b * WINDOW : (b + 1) * WINDOW, :] = jnp.concatenate(done, axis=1)


def mixed_and_normed(residual, parts, weight_ref, gain):
    width = parts[0].shape[1]
    total = residual.astype(F32)
    projected = dot32(parts[0], weight_ref[0:width])
    for j in range(1, len(parts)):
        projected = projected + dot32(parts[j], weight_ref[j * width : (j + 1) * width])
    mixed = (total + projected).astype(BF)
    wide = mixed.astype(F32)
    scale = lax.rsqrt(jnp.mean(wide * wide, axis=1, keepdims=True) + NORM_EPSILON)
    return mixed, (wide * scale * gain).astype(BF)


def dispatch_body(
    order_ref, parts_ref, residual_ref, weight_ref, gain_ref, ids_ref, pick_ref, rank_ref,
    mixed_ref, *slot_refs,
):
    own = mixed_ref.shape[0]
    start = pl.multiple_of(order_ref[0] * own, 16)
    parts = [parts_ref[j, pl.ds(start, own), :] for j in range(parts_ref.shape[0])]
    mixed, normed = mixed_and_normed(
        residual_ref[pl.ds(start, own), :], parts, weight_ref, gain_ref[...]
    )
    mixed_ref[...] = mixed
    experts = pick_ref.shape[2]
    expert_index = lax.broadcasted_iota(jnp.int32, (experts, own), 0)
    named = expert_index == ids_ref[0:1, :]
    for k in range(1, ids_ref.shape[0]):
        named = named | (expert_index == ids_ref[k : k + 1, :])
    ones = jnp.where(named, 1.0, 0.0).astype(BF)
    earlier = jnp.where(
        lax.broadcasted_iota(jnp.int32, (own, own), 0)
        < lax.broadcasted_iota(jnp.int32, (own, own), 1),
        1.0,
        0.0,
    ).astype(BF)
    ranks = jnp.where(named, dot32(ones, earlier), -1.0).astype(BF)
    for c, slot_ref in enumerate(slot_refs):
        chosen = dot32(pick_ref[c], ranks) == rank_ref[...]
        slot_ref[...] = dot32(jnp.where(chosen, 1.0, 0.0).astype(BF), normed).astype(BF)


def gated(x, gate, up):
    gate_values = dot32(x, gate)
    up_values = dot32(x, up)
    return (gate_values / (1.0 + jnp.exp(-gate_values)) * up_values).astype(BF)


def shared_body(
    order_ref, parts_ref, residual_ref, weight_ref, gain_ref, gate_ref, up_ref, down_ref,
    keep_ref, send_ref, scratch_ref,
):
    ways = parts_ref.shape[0]
    own = keep_ref.shape[1]
    parts = [parts_ref[j] for j in range(ways)]
    unused, normed = mixed_and_normed(residual_ref[...], parts, weight_ref, gain_ref[...])
    hidden = gated(normed, gate_ref[...], up_ref[...])
    scratch_ref[...] = dot32(hidden, down_ref[...]).astype(BF)
    for m in range(ways):
        start = pl.multiple_of(order_ref[m] * own, 16)
        target = keep_ref if m % 2 == 0 else send_ref
        target[m // 2] = scratch_ref[pl.ds(start, own), :]


def expert_body(*refs):
    count = (len(refs) - 3) // 2
    gate_ref, up_ref, down_ref = refs[count : count + 3]
    for x_ref, out_ref in zip(refs[:count], refs[count + 3 :]):
        hidden = gated(x_ref[...], gate_ref[...], up_ref[...])
        out_ref[...] = dot32(hidden, down_ref[...]).astype(BF)


def expert_rows(c, xs, gates, ups, downs):
    rows, width = xs[0].shape
    hid = gates.shape[2]
    whole = pl.BlockSpec((rows, width), lambda i: (0, 0))
    return pl.pallas_call(
        expert_body,
        out_shape=[jax.ShapeDtypeStruct((rows, width), BF)] * len(xs),
        grid=(1,),
        in_specs=[whole] * len(xs)
        + [
            pl.BlockSpec((None, width, hid), lambda i: (c, 0, 0)),
            pl.BlockSpec((None, width, hid), lambda i: (c, 0, 0)),
            pl.BlockSpec((None, hid, width), lambda i: (c, 0, 0)),
        ],
        out_specs=[whole] * len(xs),
        compiler_params=pltpu.CompilerParams(vmem_limit_bytes=VMEM_LIMIT),
        cost_estimate=pl.CostEstimate(
            flops=6 * rows * width * hid * len(xs),
            bytes_accessed=4 * rows * width * len(xs) + 6 * width * hid,
            transcendentals=0,
        ),
    )(*xs, gates, ups, downs)


def combine_body(last, count, ids_ref, route_ref, pick_ref, rank_ref, back_ref, *refs):
    added, out_ref = refs[:count], refs[count]
    own = ids_ref.shape[0]
    experts = pick_ref.shape[0]
    expert_index = lax.broadcasted_iota(jnp.int32, (own, experts), 1)
    weight = jnp.zeros((own, experts), F32)
    named = expert_index < 0
    for k in range(ids_ref.shape[1]):
        match = expert_index == ids_ref[:, k : k + 1]
        named = named | match
        weight = weight + jnp.where(match, route_ref[:, k : k + 1], 0.0)
    ones = jnp.where(named, 1.0, 0.0).astype(BF)
    earlier = jnp.where(
        lax.broadcasted_iota(jnp.int32, (own, own), 1)
        < lax.broadcasted_iota(jnp.int32, (own, own), 0),
        1.0,
        0.0,
    ).astype(BF)
    ranks = jnp.where(named, dot32(earlier, ones), -1.0).astype(BF)
    pick = pick_ref[...]
    chosen = dot32(ranks, pick) == rank_ref[...]
    upper = weight.astype(BF)
    lower = (weight - upper.astype(F32)).astype(BF)
    back = back_ref[...]
    total = dot32(jnp.where(chosen, dot32(upper, pick), 0.0).astype(BF), back)
    total = total + dot32(jnp.where(chosen, dot32(lower, pick), 0.0).astype(BF), back)
    for ref in added:
        total = total + ref[...].astype(F32)
    out_ref[...] = total.astype(out_ref.dtype)


def slot_tables(places_all, experts_here, capacity):
    rows = places_all * capacity
    experts_all = places_all * experts_here
    pick = np.zeros((experts_here, rows, experts_all), np.float32)
    for c in range(experts_here):
        for s in range(rows):
            pick[c, s, (s // capacity) * experts_here + c] = 1.0
    rank = (np.arange(rows) % capacity).astype(np.float32)
    return pick, rank


def per_device(
    queries,
    keys,
    values,
    sinks,
    residual,
    out_weight,
    norm_gain,
    shared_gate,
    shared_up,
    shared_down,
    expert_ids,
    route_weights,
    expert_gate,
    expert_up,
    expert_down,
):
    block_rows, query_width = queries.shape
    key_width = keys.shape[1]
    ways = lax.axis_size("tp")
    splits = lax.axis_size("sp")
    width_index = lax.axis_index("tp")
    first_row = lax.axis_index("sp") * block_rows
    total_rows = splits * block_rows
    model_width = out_weight.shape[1]
    own = block_rows // ways
    experts_here = expert_gate.shape[0]
    experts_all = experts_here * splits
    capacity = max(2, 2 * own * TOPK // experts_all)
    slots = splits * capacity

    def over(x, mask):
        return lax.ppermute(x, "tp", [(i, i ^ mask) for i in range(ways)])

    joined = jnp.concatenate([keys, values], axis=1)
    up = [(i, i + 1) for i in range(splits - 1)]
    down = [(i + 1, i) for i in range(splits - 1)]
    before = lax.ppermute(joined[block_rows - WINDOW :], "sp", up)
    after = lax.ppermute(joined[:WINDOW], "sp", down)
    places = first_row - WINDOW + jnp.arange(block_rows + 2 * WINDOW, dtype=jnp.int32)
    cosine, sine = rotary_tables(places)
    info = jnp.stack([first_row, jnp.int32(total_rows)]).astype(jnp.int32)
    attended = call(
        attention_body,
        [((block_rows, query_width), BF)],
        (queries, keys, values, before, after, cosine, sine, jnp.asarray(signed_swap(), BF)),
        scalars=(info, sinks),
        scratch=[pltpu.VMEM((key_width // HEAD_DIM, block_rows + 2 * WINDOW, HEAD_DIM), BF)] * 2,
        flops=12 * block_rows * WINDOW * query_width,
        moved=4 * block_rows * query_width,
    )[0]
    parts = lax.all_gather(attended, "tp", axis=0, tiled=False)

    order = width_index ^ jnp.arange(ways, dtype=jnp.int32)
    gain = norm_gain.reshape(1, model_width)
    own_ids = lax.dynamic_slice_in_dim(expert_ids, width_index * own, own, 0)
    pick, rank = slot_tables(splits, experts_here, capacity)
    mixed, *outgoing = call(
        dispatch_body,
        [((own, model_width), BF)] + [((slots, model_width), BF)] * experts_here,
        (
            parts,
            residual,
            out_weight,
            gain,
            own_ids.T,
            jnp.asarray(pick, BF),
            jnp.asarray(rank[:, None], F32),
        ),
        scalars=(order,),
        flops=2 * own * model_width * (out_weight.shape[0] + experts_here * slots),
        moved=2 * out_weight.size,
    )
    arrived = [lax.all_to_all(x, "sp", 0, 0, tiled=True) for x in outgoing]

    keep, send = call(
        shared_body,
        [((ways // 2, own, model_width), BF)] * 2,
        (parts, residual, out_weight, gain, shared_gate, shared_up, shared_down),
        scalars=(order,),
        scratch=[pltpu.VMEM((block_rows, model_width), BF)],
        flops=2 * block_rows * model_width * (out_weight.shape[0] + 3 * shared_gate.shape[1]),
        moved=2 * out_weight.size,
    )

    def plus(a, b):
        return (a.astype(F32) + b.astype(F32)).astype(BF)

    got = over(send, 1)
    shared_own = plus(keep[0], got[0])
    shared_far = over(plus(keep[1], got[1]), 2)

    back = []
    for c in range(experts_here):
        near = arrived[c]
        far = over(near, 2)
        near_pair = over(near, 1)
        far_pair = over(far, 1)
        out_pair, out_near = expert_rows(c, [near_pair, near], expert_gate, expert_up, expert_down)
        from_pair = over(out_pair, 1)
        out_far_pair, out_far = expert_rows(c, [far_pair, far], expert_gate, expert_up, expert_down)
        far_sum = plus(out_far, over(out_far_pair, 1))
        summed = plus(plus(out_near, from_pair), over(far_sum, 2))
        back.append(lax.all_to_all(summed, "sp", 0, 0, tiled=True))

    total = None
    for c in range(experts_here):
        last = c == experts_here - 1
        added = (mixed, shared_own, shared_far) if total is None else (total,)
        total = call(
            functools.partial(combine_body, last, len(added)),
            [((own, model_width), BF if last else F32)],
            (
                own_ids,
                route_weights,
                jnp.asarray(pick[c].T, BF),
                jnp.asarray(rank[None, :], F32),
                back[c],
                *added,
            ),
            flops=4 * own * slots * model_width,
            moved=2 * slots * model_width,
        )[0]
    return total


def solution(mesh):
    placed = (
        P("sp", "tp"),
        P("sp", "tp"),
        P("sp", "tp"),
        P("tp"),
        P("sp", None),
        P(),
        P(),
        P(None, "tp"),
        P(None, "tp"),
        P("tp", None),
        P("sp", None),
        P(("sp", "tp"), None),
        P("sp", None, "tp"),
        P("sp", None, "tp"),
        P("sp", "tp", None),
    )
    return jax.shard_map(
        per_device, mesh=mesh, in_specs=placed, out_specs=P(("sp", "tp"), None), check_vma=False
    )
```

```python
import functools

import jax
import jax.numpy as jnp
import numpy as np
from jax import lax
from jax.experimental import pallas as pl
from jax.experimental.pallas import tpu as pltpu
from jax.sharding import PartitionSpec as P

HEAD_DIM = 64
WINDOW = 128
GRID_W = 64
TOPK = 2
ROPE_BASE = 10000.0
NEG_LARGE = -1e30
NORM_EPSILON = 1e-06

BF = jnp.bfloat16
F32 = jnp.float32
VMEM_LIMIT = 56 * 1024 * 1024


def dot32(a, b):
    return jnp.dot(a, b, preferred_element_type=F32)


def call(body, outs, operands, scalars=(), scratch=(), own=(), flops=0, moved=0):
    whole = lambda shape: pl.BlockSpec(shape, lambda i, *s: (0,) * len(shape))
    specs = [whole(x.shape) for x in operands]
    for at, rows, which in own:
        index = lambda i, *s, which=which: (s[0][which], 0)
        specs[at] = pl.BlockSpec((rows, operands[at].shape[1]), index)
    operands = tuple(operands)
    grid_spec = pltpu.PrefetchScalarGridSpec(
        num_scalar_prefetch=len(scalars),
        grid=(1,),
        in_specs=specs,
        out_specs=[whole(shape) for shape, kind in outs],
        scratch_shapes=list(scratch),
    )
    return pl.pallas_call(
        body,
        out_shape=[jax.ShapeDtypeStruct(shape, kind) for shape, kind in outs],
        grid_spec=grid_spec,
        compiler_params=pltpu.CompilerParams(vmem_limit_bytes=VMEM_LIMIT),
        cost_estimate=pl.CostEstimate(flops=flops, bytes_accessed=moved, transcendentals=0),
    )(*scalars, *operands)


def attention_body(
    first_ref, sink_ref, q_ref, k_ref, v_ref, before_ref, after_ref, spectrum_ref,
    out_ref, keys_ref, values_ref, total_rows,
):
    key_width, rows = k_ref.shape
    key_heads = key_width // HEAD_DIM
    group = q_ref.shape[0] // key_width
    wide = rows + 2 * WINDOW
    quarter = HEAD_DIM // 4
    first_row = first_ref[0] * rows
    place = lax.broadcasted_iota(jnp.int32, (2 * quarter, wide), 1) + (first_row - WINDOW)
    lane_row = lax.broadcasted_iota(jnp.int32, (2 * quarter, wide), 0)
    shift = GRID_W.bit_length() - 1
    at = jnp.where(
        lane_row < quarter, lax.shift_right_arithmetic(place, shift), place & (GRID_W - 1)
    )
    angles = at.astype(F32) * spectrum_ref[...]
    cosine, sine = jnp.cos(angles), jnp.sin(angles)

    def turn(x, start):
        u = x.astype(F32)
        end = start + x.shape[1]
        pieces = []
        for half in range(2):
            c = cosine[half * quarter : (half + 1) * quarter, start:end]
            s = sine[half * quarter : (half + 1) * quarter, start:end]
            former = u[2 * half * quarter : (2 * half + 1) * quarter]
            latter = u[(2 * half + 1) * quarter : (2 * half + 2) * quarter]
            pieces.append(former * c - latter * s)
            pieces.append(former * s + latter * c)
        return jnp.concatenate(pieces, axis=0)

    query_index = lax.broadcasted_iota(jnp.int32, (3 * WINDOW, WINDOW), 1)
    key_index = lax.broadcasted_iota(jnp.int32, (3 * WINDOW, WINDOW), 0)
    apart = key_index - query_index
    near = (apart >= 0) & (apart <= 2 * WINDOW)
    blocks = rows // WINDOW
    finished = [[] for _ in range(blocks)]
    for g in range(key_heads):
        cut = slice(g * HEAD_DIM, (g + 1) * HEAD_DIM)
        late = slice(key_width + g * HEAD_DIM, key_width + (g + 1) * HEAD_DIM)
        keys = jnp.concatenate([before_ref[cut], k_ref[cut], after_ref[cut]], axis=1)
        keys_ref[...] = turn(keys, 0).T.astype(BF)
        values_ref[...] = jnp.concatenate([before_ref[late], v_ref[cut], after_ref[late]], axis=1)
        turned = [
            turn(q_ref[h * HEAD_DIM : (h + 1) * HEAD_DIM], WINDOW).astype(BF)
            for h in range(g * group, (g + 1) * group)
        ]
        sink = jnp.concatenate(
            [jnp.full((1, WINDOW), sink_ref[h], F32) for h in range(g * group, (g + 1) * group)],
            axis=1,
        )
        for b in range(blocks):
            key_at = key_index + (first_row + (b - 1) * WINDOW)
            allowed = near & (key_at >= 0) & (key_at < total_rows)
            penalty = jnp.where(allowed, 0.0, NEG_LARGE)
            penalty = jnp.concatenate([penalty] * group, axis=1)
            heads = jnp.concatenate(
                [q[:, b * WINDOW : (b + 1) * WINDOW] for q in turned], axis=1
            )
            scores = dot32(keys_ref[b * WINDOW : (b + 3) * WINDOW], heads)
            scores = scores * HEAD_DIM ** (-0.5) + penalty
            highest = jnp.maximum(jnp.max(scores, axis=0, keepdims=True), sink)
            lifted = jnp.exp(scores - highest)
            denominator = jnp.sum(lifted, axis=0, keepdims=True) + jnp.exp(sink - highest)
            probabilities = (lifted * (1.0 / denominator)).astype(BF)
            result = dot32(values_ref[:, b * WINDOW : (b + 3) * WINDOW], probabilities)
            for i in range(group):
                finished[b].append(result[:, i * WINDOW : (i + 1) * WINDOW].T.astype(BF))
    for b in range(blocks):
        out_ref[b * WINDOW : (b + 1) * WINDOW, :] = jnp.concatenate(finished[b], axis=1)


def mixed_and_normed(residual, parts, weight, gain):
    mixed = (residual.astype(F32) + dot32(parts, weight)).astype(BF)
    wide = mixed.astype(F32)
    scale = lax.rsqrt(jnp.mean(wide * wide, axis=1, keepdims=True) + NORM_EPSILON)
    return mixed, (wide * scale * gain).astype(BF)


def ranks_of(ids_ref, block, experts):
    own = ids_ref.shape[2]
    expert_index = lax.broadcasted_iota(jnp.int32, (experts, own), 0)
    ids = ids_ref[block]
    named = expert_index == ids[0:1, :]
    for k in range(1, ids.shape[0]):
        named = named | (expert_index == ids[k : k + 1, :])
    ones = jnp.where(named, 1.0, 0.0).astype(BF)
    earlier = jnp.where(
        lax.broadcasted_iota(jnp.int32, (own, own), 0)
        < lax.broadcasted_iota(jnp.int32, (own, own), 1),
        1.0,
        0.0,
    ).astype(BF)
    return jnp.where(named, dot32(ones, earlier), -1.0).astype(BF)


def slot_choice(ranks, place, rank, turn, experts_here, c):
    experts = ranks.shape[0]
    wanted = (place ^ turn) * experts_here + c
    shape = (place.shape[0], experts)
    pick = jnp.where(lax.broadcasted_iota(jnp.int32, shape, 1) == wanted, 1.0, 0.0).astype(BF)
    return jnp.where(dot32(pick, ranks) == rank, 1.0, 0.0).astype(BF)


def dispatch_body(
    order_ref, parts_ref, residual_ref, weight_ref, gain_ref, ids_ref, place_ref, rank_ref,
    mixed_ref, slot_ref, experts,
):
    own = mixed_ref.shape[0]
    start = pl.multiple_of(order_ref[0] * own, 16)
    parts = [parts_ref[j, pl.ds(start, own), :] for j in range(parts_ref.shape[0])]
    parts = jnp.concatenate(parts, axis=1)
    mixed, normed = mixed_and_normed(residual_ref[...], parts, weight_ref[...], gain_ref[...])
    mixed_ref[...] = mixed
    ranks = ranks_of(ids_ref, order_ref[0], experts[0])
    chosen = slot_choice(ranks, place_ref[...], rank_ref[...], 0, experts[1], 0)
    slot_ref[...] = dot32(chosen, normed).astype(BF)


def gated(x, gate, up):
    gate_values = dot32(x, gate)
    up_values = dot32(x, up)
    return (gate_values / (1.0 + jnp.exp(-gate_values)) * up_values).astype(BF)


def second_body(
    order_ref, turn_ref, parts_ref, near_ref, far_ref, weight_ref, gain_ref, ids_ref,
    place_ref, rank_ref, *slot_refs, experts,
):
    ways = parts_ref.shape[0]
    own = near_ref.shape[0]
    blocks = []
    for m in range(0, ways, 2):
        start = pl.multiple_of(order_ref[m] * own, 16)
        parts = [parts_ref[j, pl.ds(start, own), :] for j in range(ways)]
        blocks.append(jnp.concatenate(parts, axis=1))
    residual = jnp.concatenate([near_ref[...], far_ref[...]], axis=0)
    _, normed = mixed_and_normed(
        residual, jnp.concatenate(blocks, axis=0), weight_ref[...], gain_ref[...]
    )
    pieces = len(slot_refs) // (experts[1] - 1)
    for m in range(0, ways, 2):
        ranks = ranks_of(ids_ref, order_ref[m], experts[0])
        rows = normed[(m // 2) * own : (m // 2 + 1) * own]
        for c in range(1, experts[1]):
            chosen = slot_choice(
                ranks, place_ref[...], rank_ref[...], turn_ref[0], experts[1], c
            )
            result = dot32(chosen, rows)
            for p in range(pieces):
                slots_ref = slot_refs[(c - 1) * pieces + p]
                count = slots_ref.shape[0] // (ways // 2)
                slots_ref[(m // 2) * count : (m // 2 + 1) * count] = result[
                    p * count : (p + 1) * count
                ].astype(BF)


def shared_body(
    order_ref, parts_ref, residual_ref, weight_ref, gain_ref, gate_ref, up_ref, down_ref,
    keep_ref, send_ref, scratch_ref,
):
    ways = parts_ref.shape[0]
    own = keep_ref.shape[1]
    parts = jnp.concatenate([parts_ref[j] for j in range(ways)], axis=1)
    _, normed = mixed_and_normed(
        residual_ref[...], parts, weight_ref[...], gain_ref[...]
    )
    hidden = gated(normed, gate_ref[...], up_ref[...])
    scratch_ref[...] = dot32(hidden, down_ref[...]).astype(BF)
    for m in range(ways):
        start = pl.multiple_of(order_ref[m] * own, 16)
        target = keep_ref if m % 2 == 0 else send_ref
        target[m // 2] = scratch_ref[pl.ds(start, own), :]


def expert_body(c, count, *refs):
    xs, (gate_hbm, up_hbm, down_hbm) = refs[:count], refs[count : count + 3]
    outs = refs[count + 3 : 2 * count + 3]
    x_buf, gate, up, down, out_buf, sems = refs[2 * count + 3 :]
    loads = [
        pltpu.make_async_copy(gate_hbm.at[c], gate, sems.at[0]),
        pltpu.make_async_copy(up_hbm.at[c], up, sems.at[1]),
        pltpu.make_async_copy(down_hbm.at[c], down, sems.at[2]),
    ]
    reads = [
        pltpu.make_async_copy(xs[i], x_buf.at[i], sems.at[3 + i]) for i in range(count)
    ]
    writes = [
        pltpu.make_async_copy(out_buf.at[i], outs[i], sems.at[3 + count + i])
        for i in range(count)
    ]
    reads[0].start()
    loads[0].start()
    loads[1].start()
    loads[2].start()
    for i in range(1, count):
        reads[i].start()
    reads[0].wait()
    loads[0].wait()
    for i in range(count):
        if i:
            reads[i].wait()
        gate_values = dot32(x_buf[i], gate[...])
        if i == 0:
            loads[1].wait()
        up_values = dot32(x_buf[i], up[...])
        hidden = (gate_values / (1.0 + jnp.exp(-gate_values)) * up_values).astype(BF)
        if i == 0:
            loads[2].wait()
        out_buf[i] = dot32(hidden, down[...]).astype(BF)
        writes[i].start()
    for i in range(count):
        writes[i].wait()


def expert_rows(c, xs, gates, ups, downs):
    rows, width = xs[0].shape
    hid = gates.shape[2]
    count = len(xs)
    hbm = pl.BlockSpec(memory_space=pltpu.HBM)
    return pl.pallas_call(
        functools.partial(expert_body, c, count),
        out_shape=[jax.ShapeDtypeStruct((rows, width), BF)] * count,
        in_specs=[hbm] * (count + 3),
        out_specs=[hbm] * count,
        scratch_shapes=[
            pltpu.VMEM((count, rows, width), BF),
            pltpu.VMEM((width, hid), BF),
            pltpu.VMEM((width, hid), BF),
            pltpu.VMEM((hid, width), BF),
            pltpu.VMEM((count, rows, width), BF),
            pltpu.SemaphoreType.DMA((3 + 2 * count,)),
        ],
        compiler_params=pltpu.CompilerParams(vmem_limit_bytes=VMEM_LIMIT),
        cost_estimate=pl.CostEstimate(
            flops=6 * rows * width * hid * count,
            bytes_accessed=4 * rows * width * count + 6 * width * hid,
            transcendentals=0,
        ),
    )(*xs, gates, ups, downs)


def joined_body(count, *refs):
    pieces, outs = refs[:count], refs[count:]
    rows = outs[0].shape[0] // count
    for p, piece in enumerate(pieces):
        for h, out in enumerate(outs):
            out[p * rows : (p + 1) * rows] = piece[h * rows : (h + 1) * rows]


def joined(pieces, halves):
    rows, width = pieces[0].shape
    count = len(pieces)
    return call(
        functools.partial(joined_body, count),
        [((count * rows // halves, width), BF)] * halves,
        pieces,
        flops=rows * width * count,
        moved=4 * rows * width * count,
    )


def prepare_body(
    order_ref, turn_ref, ids_ref, route_ref, place_ref, rank_ref, out_ref, experts,
):
    own = ids_ref.shape[0]
    expert_index = lax.broadcasted_iota(jnp.int32, (own, experts[0]), 1)
    weight = jnp.zeros((own, experts[0]), F32)
    named = expert_index < 0
    for k in range(ids_ref.shape[1]):
        match = expert_index == ids_ref[:, k : k + 1]
        named = named | match
        weight = weight + jnp.where(match, route_ref[:, k : k + 1], 0.0)
    ones = jnp.where(named, 1.0, 0.0).astype(BF)
    earlier = jnp.where(
        lax.broadcasted_iota(jnp.int32, (own, own), 1)
        < lax.broadcasted_iota(jnp.int32, (own, own), 0),
        1.0,
        0.0,
    ).astype(BF)
    ranks = jnp.where(named, dot32(earlier, ones), -1.0).astype(BF)
    upper = weight.astype(BF)
    lower = (weight - upper.astype(F32)).astype(BF)
    shape = (experts[0], place_ref.shape[1])
    row_index = lax.broadcasted_iota(jnp.int32, shape, 0)
    wanted = (place_ref[...] ^ turn_ref[0]) * experts[1] + experts[2]
    pick = jnp.where(row_index == wanted, 1.0, 0.0).astype(BF)
    chosen = dot32(ranks, pick) == rank_ref[...]
    out_ref[0] = jnp.where(chosen, dot32(upper, pick), 0.0).astype(BF)
    out_ref[1] = jnp.where(chosen, dot32(lower, pick), 0.0).astype(BF)


def combine_body(count, weights_ref, *refs):
    back_ref = refs[-1]
    rows = back_ref.shape[0] // count
    for p in range(count):
        back_ref[p * rows : (p + 1) * rows] = refs[p][...]
    back = back_ref[...]
    total = dot32(weights_ref[0], back) + dot32(weights_ref[1], back)
    for ref in refs[count:-2]:
        total = total + ref[...].astype(F32)
    refs[-2][...] = total.astype(refs[-2].dtype)


def layer(
    queries,
    keys,
    values,
    sinks,
    residual,
    out_weight,
    norm_gain,
    shared_gate,
    shared_up,
    shared_down,
    expert_ids,
    route_weights,
    expert_gate,
    expert_up,
    expert_down,
):
    block_rows, query_width = queries.shape
    ways = lax.axis_size("tp")
    splits = lax.axis_size("sp")
    width_index = lax.axis_index("tp")
    sp_index = lax.axis_index("sp")
    model_width = out_weight.shape[1]
    own = block_rows // ways
    halves = ways // 2
    experts_here = expert_gate.shape[0]
    experts_all = experts_here * splits
    capacity = max(2, 2 * own * TOPK // experts_all)
    slots = splits * capacity

    def over(x, mask):
        return lax.ppermute(x, "tp", [(i, i ^ mask) for i in range(ways)])

    def exchange(x):
        return lax.all_to_all(x, "sp", 0, 0, tiled=True)

    def turned(pieces, masks):
        done = []
        for piece, m in zip(pieces, masks):
            pairs = [(i, i ^ m) for i in range(splits)]
            done.append(lax.ppermute(piece, "sp", pairs) if m else piece)
        return done

    def returned(keep, send, name, first):
        if not turning:
            summed = plus(keep, over(send, 2))
            return [exchange(summed)]
        half = splits // 2
        rows = half * capacity
        pieces = [None] * splits
        for part in (1, 0):
            start = rows * (part ^ first)
            mine = lax.dynamic_slice_in_dim(keep, start, rows, 0)
            other = lax.dynamic_slice_in_dim(send, start, rows, 0)
            other = over(other, 2)
            if part == 0:
                other, summed = lax.optimization_barrier((other, summed))
            summed = plus(mine, other)
            masks = range(part * half, (part + 1) * half)
            for m in masks:
                inner = (m % half) ^ first_low[name]
                pieces[m] = lax.dynamic_slice_in_dim(summed, inner * capacity, capacity, 0)
            pieces[part * half : (part + 1) * half] = turned(
                pieces[part * half : (part + 1) * half], masks
            )
        return pieces

    def plus(a, b):
        return (a.astype(F32) + b.astype(F32)).astype(BF)

    up = [(i, i + 1) for i in range(splits - 1)]
    down = [(i + 1, i) for i in range(splits - 1)]
    keys_t, values_t = keys.T, values.T
    tail = jnp.concatenate([keys_t[:, -WINDOW:], values_t[:, -WINDOW:]], axis=0)
    head = jnp.concatenate([keys_t[:, :WINDOW], values_t[:, :WINDOW]], axis=0)
    before = lax.ppermute(tail, "sp", up)
    after = lax.ppermute(head, "sp", down)
    quarter = HEAD_DIM // 4
    spectrum = ROPE_BASE ** (-np.arange(quarter, dtype=np.float64) / quarter)
    spectrum = np.concatenate([spectrum, spectrum])[:, None].astype(np.float32)
    attended = call(
        functools.partial(attention_body, total_rows=splits * block_rows),
        [((block_rows, query_width), BF)],
        (queries.T, keys_t, values_t, before, after, jnp.asarray(spectrum)),
        scalars=(sp_index.reshape(1), sinks),
        scratch=[
            pltpu.VMEM((block_rows + 2 * WINDOW, HEAD_DIM), BF),
            pltpu.VMEM((HEAD_DIM, block_rows + 2 * WINDOW), BF),
        ],
        flops=12 * block_rows * WINDOW * query_width,
        moved=4 * block_rows * query_width,
    )[0]

    order = width_index ^ jnp.arange(ways, dtype=jnp.int32)
    gain = norm_gain.reshape(1, model_width)
    ids_t = expert_ids.T.reshape(TOPK, ways, own).transpose(1, 0, 2)
    experts = (experts_all, experts_here)
    place = np.arange(slots, dtype=np.int32) // capacity
    rank = (np.arange(slots) % capacity).astype(np.float32)
    turning = splits <= 8
    turn = (sp_index if turning else sp_index * 0).reshape(1)
    combine_weights = []
    for c in range(experts_here):
        combine_weights += call(
            functools.partial(prepare_body, experts=(*experts, c)),
            [((2, own, slots), BF)],
            (expert_ids, route_weights, jnp.asarray(place[None, :]), jnp.asarray(rank[None, :])),
            scalars=(order, turn),
            own=((0, own, 0),),
            flops=4 * own * experts_all * slots,
            moved=4 * own * slots,
        )
    parts = lax.all_gather(attended, "tp", axis=0, tiled=False)
    mixed, outgoing = call(
        functools.partial(dispatch_body, experts=experts),
        [((own, model_width), BF), ((slots, model_width), BF)],
        (
            parts,
            residual,
            out_weight,
            gain,
            ids_t,
            jnp.asarray(place[:, None]),
            jnp.asarray(rank[:, None]),
        ),
        scalars=(order,),
        own=((1, own, 0),),
        flops=2 * own * model_width * (out_weight.shape[0] + slots),
        moved=2 * out_weight.size,
    )
    near = exchange(outgoing)

    outgoing = call(
        functools.partial(second_body, experts=experts),
        [((halves * capacity, model_width), BF)] * (splits * (experts_here - 1)),
        (
            parts,
            residual,
            residual,
            out_weight,
            gain,
            ids_t,
            jnp.asarray(place[:, None]),
            jnp.asarray(rank[:, None]),
        ),
        scalars=(order, turn),
        own=((1, own, 0), (2, own, 2)),
        flops=2 * halves * own * model_width * (out_weight.shape[0] + slots),
        moved=2 * out_weight.size,
    )
    keep, send = call(
        shared_body,
        [((halves, own, model_width), BF)] * 2,
        (parts, residual, out_weight, gain, shared_gate, shared_up, shared_down),
        scalars=(order,),
        scratch=[pltpu.VMEM((block_rows, model_width), BF)],
        flops=2 * block_rows * model_width * (out_weight.shape[0] + 3 * shared_gate.shape[1]),
        moved=2 * out_weight.size,
    )
    got = over(send, 1)
    shared_own = plus(keep[0], got[0])
    shared_far = over(plus(keep[1], got[1]), 2)

    weights = (expert_gate, expert_up, expert_down)
    far = over(near, 2)
    near_pair = over(near, 1)
    far_pair = over(far, 1)
    out_pair, out_near = expert_rows(0, [near_pair, near], *weights)
    from_pair = over(out_pair, 1)
    out_far_pair, out_far = expert_rows(0, [far_pair, far], *weights)
    far_sum = plus(out_far, over(out_far_pair, 1))
    near_sum = plus(out_near, from_pair)
    half = splits // 2
    first_low = {"near": sp_index % half, "mine": 0}
    back = [returned(near_sum, far_sum, "near", sp_index // half)]

    for c in range(1, experts_here):
        pieces = outgoing[splits * (c - 1) : splits * c]
        if turning:
            arrived = turned(pieces, range(splits))
            mine, far = joined(arrived, halves)
        else:
            arrived = exchange(jnp.concatenate(pieces, axis=0))
            arrived = arrived.reshape(splits, halves, capacity, model_width)
            mine, far = (arrived[:, h].reshape(slots, model_width) for h in range(halves))
        far_pair = over(far, 1)
        out_pair, out_far = expert_rows(c, [far_pair, far], *weights)
        far_sum = plus(out_far, over(out_pair, 1))
        pair = over(mine, 1)
        out_pair, out_mine = expert_rows(c, [pair, mine], *weights)
        summed = plus(out_mine, over(out_pair, 1))
        back.append(returned(summed, far_sum, "mine", 0))

    total = None
    for c in range(experts_here):
        last = c == experts_here - 1
        added = (mixed, shared_own, shared_far) if total is None else (total,)
        total = call(
            functools.partial(combine_body, len(back[c])),
            [((own, model_width), BF if last else F32)],
            (combine_weights[c], *back[c], *added),
            scratch=[pltpu.VMEM((slots, model_width), BF)],
            flops=4 * own * slots * model_width,
            moved=2 * slots * model_width,
        )[0]
    return total


def solution(mesh):
    placed = (
        P("sp", "tp"),
        P("sp", "tp"),
        P("sp", "tp"),
        P("tp"),
        P("sp", None),
        P(),
        P(),
        P(None, "tp"),
        P(None, "tp"),
        P("tp", None),
        P("sp", None),
        P(("sp", "tp"), None),
        P("sp", None, "tp"),
        P("sp", None, "tp"),
        P("sp", "tp", None),
    )
    return jax.shard_map(
        layer, mesh=mesh, in_specs=placed, out_specs=P(("sp", "tp"), None), check_vma=False
    )
```

```python
import functools

import jax
import jax.numpy as jnp
import numpy as np
from jax import lax
from jax.experimental import pallas as pl
from jax.experimental.pallas import tpu as pltpu
from jax.sharding import PartitionSpec as P

HEAD_DIM = 64
WINDOW = 128
GRID_W = 64
TOPK = 2
ROPE_BASE = 10000.0
NEG_LARGE = -1e30
NORM_EPSILON = 1e-06

BF = jnp.bfloat16
F32 = jnp.float32
VMEM_LIMIT = 20 * 1024 * 1024


def dot32(a, b):
    return jnp.dot(a, b, preferred_element_type=F32)


def call(body, outs, operands, scalars=(), scratch=(), flops=0, moved=0, final=False):
    local = pl.BlockSpec(memory_space=pltpu.VMEM)
    grid_spec = pltpu.PrefetchScalarGridSpec(
        num_scalar_prefetch=len(scalars),
        grid=(),
        in_specs=[local] * len(operands),
        out_specs=[local] * len(outs),
        scratch_shapes=list(scratch),
    )
    shape_of = jax.ShapeDtypeStruct if final else pltpu.VMEM
    return pl.pallas_call(
        body,
        out_shape=[shape_of(shape, kind) for shape, kind in outs],
        grid_spec=grid_spec,
        compiler_params=pltpu.CompilerParams(vmem_limit_bytes=VMEM_LIMIT),
        cost_estimate=pl.CostEstimate(flops=flops, bytes_accessed=moved, transcendentals=0),
    )(*scalars, *(pltpu.with_memory_space_constraint(x, pltpu.VMEM) for x in operands))


def attention_body(
    tp_ref, first_ref, sink_ref, q_ref, k_ref, v_ref, before_ref, after_ref, spectrum_ref,
    *refs, total_rows,
):
    outs, (out_ref, keys_ref, values_ref) = refs[:-3], refs[-3:]
    key_width, rows = k_ref.shape
    key_heads = key_width // HEAD_DIM
    group = q_ref.shape[0] // key_width
    wide = rows + 2 * WINDOW
    quarter = HEAD_DIM // 4
    first_row = first_ref[0] * rows
    place = lax.broadcasted_iota(jnp.int32, (2 * quarter, wide), 1) + (first_row - WINDOW)
    lane_row = lax.broadcasted_iota(jnp.int32, (2 * quarter, wide), 0)
    shift = GRID_W.bit_length() - 1
    at = jnp.where(
        lane_row < quarter, lax.shift_right_arithmetic(place, shift), place & (GRID_W - 1)
    )
    angles = at.astype(F32) * spectrum_ref[...]
    cosine, sine = jnp.cos(angles), jnp.sin(angles)

    def turn(x, start):
        u = x.astype(F32)
        end = start + x.shape[1]
        pieces = []
        for half in range(2):
            c = cosine[half * quarter : (half + 1) * quarter, start:end]
            s = sine[half * quarter : (half + 1) * quarter, start:end]
            former = u[2 * half * quarter : (2 * half + 1) * quarter]
            latter = u[(2 * half + 1) * quarter : (2 * half + 2) * quarter]
            pieces.append(former * c - latter * s)
            pieces.append(former * s + latter * c)
        return jnp.concatenate(pieces, axis=0)

    query_index = lax.broadcasted_iota(jnp.int32, (3 * WINDOW, WINDOW), 1)
    key_index = lax.broadcasted_iota(jnp.int32, (3 * WINDOW, WINDOW), 0)
    apart = key_index - query_index
    near = (apart >= 0) & (apart <= 2 * WINDOW)
    blocks = rows // WINDOW
    finished = [[] for _ in range(blocks)]
    for g in range(key_heads):
        cut = slice(g * HEAD_DIM, (g + 1) * HEAD_DIM)
        late = slice(key_width + g * HEAD_DIM, key_width + (g + 1) * HEAD_DIM)
        keys = jnp.concatenate([before_ref[cut], k_ref[cut], after_ref[cut]], axis=1)
        keys_ref[...] = turn(keys, 0).T.astype(BF)
        values_ref[...] = jnp.concatenate([before_ref[late], v_ref[cut], after_ref[late]], axis=1)
        turned = [
            turn(q_ref[h * HEAD_DIM : (h + 1) * HEAD_DIM], WINDOW).astype(BF)
            for h in range(g * group, (g + 1) * group)
        ]
        sink = jnp.concatenate(
            [jnp.full((1, WINDOW), sink_ref[h], F32) for h in range(g * group, (g + 1) * group)],
            axis=1,
        )
        for b in range(blocks):
            key_at = key_index + (first_row + (b - 1) * WINDOW)
            allowed = near & (key_at >= 0) & (key_at < total_rows)
            penalty = jnp.where(allowed, 0.0, NEG_LARGE)
            penalty = jnp.concatenate([penalty] * group, axis=1)
            heads = jnp.concatenate(
                [q[:, b * WINDOW : (b + 1) * WINDOW] for q in turned], axis=1
            )
            scores = dot32(keys_ref[b * WINDOW : (b + 3) * WINDOW], heads)
            scores = scores * HEAD_DIM ** (-0.5) + penalty
            highest = jnp.maximum(jnp.max(scores, axis=0, keepdims=True), sink)
            lifted = jnp.exp(scores - highest)
            denominator = jnp.sum(lifted, axis=0, keepdims=True) + jnp.exp(sink - highest)
            probabilities = (lifted * (1.0 / denominator)).astype(BF)
            result = dot32(values_ref[:, b * WINDOW : (b + 3) * WINDOW], probabilities)
            for i in range(group):
                finished[b].append(result[:, i * WINDOW : (i + 1) * WINDOW].T.astype(BF))
    for b in range(blocks):
        out_ref[b * WINDOW : (b + 1) * WINDOW, :] = jnp.concatenate(finished[b], axis=1)
    ways = len(outs) // 2
    own = rows // ways
    blocks = [out_ref[pl.ds(pl.multiple_of((tp_ref[0] ^ m) * own, 16), own), :] for m in range(ways)]
    for m in range(ways):
        outs[m][...] = blocks[m]
        for n in range(1, ways):
            outs[ways + m][(n - 1) * own : n * own] = blocks[m ^ n]


def mixed_and_normed(residual, parts, weight, gain):
    mixed = (residual.astype(F32) + dot32(parts, weight)).astype(BF)
    wide = mixed.astype(F32)
    scale = lax.rsqrt(jnp.mean(wide * wide, axis=1, keepdims=True) + NORM_EPSILON)
    return mixed, (wide * scale * gain).astype(BF)


def block_ids(ids_ref, block, own):
    rows = ids_ref.shape[1]
    return pltpu.roll(ids_ref[...], lax.rem(rows - block * own, rows), 1)[:, :own]


def ranks_of(ids, experts):
    own = ids.shape[1]
    expert_index = lax.broadcasted_iota(jnp.int32, (experts, own), 0)
    named = expert_index == ids[0:1, :]
    for k in range(1, ids.shape[0]):
        named = named | (expert_index == ids[k : k + 1, :])
    ones = jnp.where(named, 1.0, 0.0).astype(BF)
    earlier = jnp.where(
        lax.broadcasted_iota(jnp.int32, (own, own), 0)
        < lax.broadcasted_iota(jnp.int32, (own, own), 1),
        1.0,
        0.0,
    ).astype(BF)
    return jnp.where(named, dot32(ones, earlier), -1.0).astype(BF)


def slot_choice(ranks, place, rank, turn, experts_here, c):
    experts = ranks.shape[0]
    wanted = (place ^ turn) * experts_here + c
    shape = (place.shape[0], experts)
    pick = jnp.where(lax.broadcasted_iota(jnp.int32, shape, 1) == wanted, 1.0, 0.0).astype(BF)
    return jnp.where(dot32(pick, ranks) == rank, 1.0, 0.0).astype(BF)


def dispatch_body(ways, tp_ref, turn_ref, *refs, experts):
    parts, (residual_ref, weight_ref, gain_ref, ids_ref, place_ref, rank_ref) = (
        refs[:ways],
        refs[ways : ways + 6],
    )
    mixed_ref, slot_refs = refs[ways + 6], refs[ways + 7 :]
    own = mixed_ref.shape[0]
    parts = jnp.concatenate([part[...] for part in parts], axis=1)
    mixed, normed = mixed_and_normed(
        residual_ref[:own], parts, weight_ref[...], gain_ref[...]
    )
    mixed_ref[...] = mixed
    ranks = ranks_of(block_ids(ids_ref, tp_ref[0], own), experts[0])
    chosen = slot_choice(ranks, place_ref[...], rank_ref[...], turn_ref[0], experts[1], 0)
    result = dot32(chosen, normed)
    for p, slot_ref in enumerate(slot_refs):
        count = slot_ref.shape[0]
        slot_ref[...] = result[p * count : (p + 1) * count].astype(BF)


def gated(x, gate, up):
    gate_values = dot32(x, gate)
    up_values = dot32(x, up)
    return (gate_values / (1.0 + jnp.exp(-gate_values)) * up_values).astype(BF)


def second_body(ways, tp_ref, turn_ref, *refs, experts):
    parts, rests = refs[:ways], refs[ways : 2 * ways]
    residual_ref, weight_ref, gain_ref, ids_ref, place_ref, rank_ref = refs[
        2 * ways : 2 * ways + 6
    ]
    slot_refs = refs[2 * ways + 6 :]
    own = residual_ref.shape[0] // ways
    blocks, residual = [], []
    for m in range(0, ways, 2):
        rows = [rest[(m - 1) * own : m * own] for rest in rests] if m else [
            part[...] for part in parts
        ]
        blocks.append(jnp.concatenate(rows, axis=1))
        residual.append(residual_ref[m * own : (m + 1) * own])
    blocks, residual = jnp.concatenate(blocks, axis=0), jnp.concatenate(residual, axis=0)
    _, normed = mixed_and_normed(residual, blocks, weight_ref[...], gain_ref[...])
    pieces = len(slot_refs) // (experts[1] - 1)
    for m in range(0, ways, 2):
        ranks = ranks_of(block_ids(ids_ref, tp_ref[0] ^ m, own), experts[0])
        rows = normed[(m // 2) * own : (m // 2 + 1) * own]
        for c in range(1, experts[1]):
            chosen = slot_choice(
                ranks, place_ref[...], rank_ref[...], turn_ref[0], experts[1], c
            )
            result = dot32(chosen, rows)
            for p in range(pieces):
                slots_ref = slot_refs[(c - 1) * pieces + p]
                count = slots_ref.shape[0] // (ways // 2)
                slots_ref[(m // 2) * count : (m // 2 + 1) * count] = result[
                    p * count : (p + 1) * count
                ].astype(BF)


def shared_body(ways, *refs):
    parts, rests = refs[:ways], refs[ways : 2 * ways]
    residual_ref, weight_ref, gain_ref, gate_ref, up_ref, down_ref = refs[
        2 * ways : 2 * ways + 6
    ]
    keep_ref, send_ref = refs[2 * ways + 6 :]
    own = keep_ref.shape[1]
    rows = [
        jnp.concatenate([part[...], rest[...]], axis=0) for part, rest in zip(parts, rests)
    ]
    _, normed = mixed_and_normed(
        residual_ref[...], jnp.concatenate(rows, axis=1), weight_ref[...], gain_ref[...]
    )
    hidden = gated(normed, gate_ref[...], up_ref[...])
    result = dot32(hidden, down_ref[...]).astype(BF)
    for m in range(ways):
        target = keep_ref if m % 2 == 0 else send_ref
        target[m // 2] = result[m * own : (m + 1) * own]


def expert_body(c, count, *refs):
    gate_ref, up_ref, down_ref = refs[count : count + 3]
    for x_ref, out_ref in zip(refs[:count], refs[count + 3 :]):
        hidden = gated(x_ref[...], gate_ref[c], up_ref[c])
        out_ref[...] = dot32(hidden, down_ref[c]).astype(BF)


def expert_rows(c, xs, gates, ups, downs):
    rows, width = xs[0].shape
    hid = gates.shape[2]
    count = len(xs)
    return call(
        functools.partial(expert_body, c, count),
        [((rows, width), BF)] * count,
        (*xs, gates, ups, downs),
        flops=6 * rows * width * hid * count,
        moved=4 * rows * width * count + 6 * width * hid,
    )


def marker_body(x_ref, out_ref):
    out_ref[...] = x_ref[...]


def marker(x):
    return call(marker_body, [(x.shape, x.dtype)], (x,), flops=1000, moved=1000)[0]


def joined_body(count, *refs):
    pieces, outs = refs[:count], refs[count:]
    rows = outs[0].shape[0] // count
    for p, piece in enumerate(pieces):
        for h, out in enumerate(outs):
            out[p * rows : (p + 1) * rows] = piece[h * rows : (h + 1) * rows]


def joined(pieces, halves=1):
    rows, width = pieces[0].shape
    count = len(pieces)
    return call(
        functools.partial(joined_body, count),
        [((count * rows // halves, width), BF)] * halves,
        pieces,
        flops=rows * width * count,
        moved=4 * rows * width * count,
    )


def prepare_body(
    tp_ref, turn_ref, ids_ref, route_ref, place_ref, rank_ref, *out_refs, experts,
):
    own = route_ref.shape[1]
    ids = block_ids(ids_ref, tp_ref[0], own)
    ranks = ranks_of(ids, experts[0])
    expert_index = lax.broadcasted_iota(jnp.int32, (experts[0], own), 0)
    weight = jnp.zeros((experts[0], own), F32)
    for k in range(ids.shape[0]):
        weight = weight + jnp.where(
            expert_index == ids[k : k + 1, :], route_ref[k : k + 1, :], 0.0
        )
    upper = weight.astype(BF)
    lower = (weight - upper.astype(F32)).astype(BF)
    row_index = lax.broadcasted_iota(jnp.int32, (experts[0], place_ref.shape[1]), 0)

    def spread(x, pick):
        return lax.dot_general(x, pick, (((0,), (0,)), ((), ())), preferred_element_type=F32)

    for c, out_ref in enumerate(out_refs):
        wanted = (place_ref[...] ^ turn_ref[0]) * experts[1] + c
        pick = jnp.where(row_index == wanted, 1.0, 0.0).astype(BF)
        chosen = spread(ranks, pick) == rank_ref[...]
        out_ref[0] = jnp.where(chosen, spread(upper, pick), 0.0).astype(BF)
        out_ref[1] = jnp.where(chosen, spread(lower, pick), 0.0).astype(BF)


def load_body(count, ways, tp_ref, *refs):
    sources, outs, sems = refs[:count], refs[-1 - count : -1], refs[-1]
    copies = []
    for source, out in zip(sources, outs):
        rows = source.shape[0] // ways
        for m in range(ways):
            cut = (
                pl.ds(pl.multiple_of((tp_ref[0] ^ m) * rows, 16), rows) if ways > 1 else pl.ds(0, rows)
            )
            copies.append(
                pltpu.make_async_copy(
                    source.at[cut], out.at[pl.ds(m * rows, rows)], sems.at[len(copies)]
                )
            )
    for copy in copies:
        copy.start()
    for copy in copies:
        copy.wait()


def load(arrays, after, tp, ways):
    hbm = pl.BlockSpec(memory_space=pltpu.HBM)
    return pl.pallas_call(
        functools.partial(load_body, len(arrays), ways),
        out_shape=[pltpu.VMEM(x.shape, x.dtype) for x in arrays],
        grid_spec=pltpu.PrefetchScalarGridSpec(
            num_scalar_prefetch=1,
            grid=(),
            in_specs=[hbm] * (len(arrays) + len(after)),
            out_specs=[pl.BlockSpec(memory_space=pltpu.VMEM)] * len(arrays),
            scratch_shapes=[pltpu.SemaphoreType.DMA((len(arrays) * ways,))],
        ),
        compiler_params=pltpu.CompilerParams(vmem_limit_bytes=1024 * 1024),
        cost_estimate=pl.CostEstimate(
            flops=1000, bytes_accessed=sum(2 * x.size for x in arrays), transcendentals=0
        ),
    )(tp, *(pltpu.with_memory_space_constraint(x, pltpu.HBM) for x in (*arrays, *after)))


def combine_body(count, weights_ref, *refs):
    back_ref = refs[-1]
    rows = back_ref.shape[0] // count
    for p in range(count):
        back_ref[p * rows : (p + 1) * rows] = refs[p][...]
    back = back_ref[...]
    total = dot32(weights_ref[0], back) + dot32(weights_ref[1], back)
    for ref in refs[count:-2]:
        total = total + ref[...].astype(F32)
    refs[-2][...] = total.astype(refs[-2].dtype)


def layer(
    queries,
    keys,
    values,
    sinks,
    residual,
    out_weight,
    norm_gain,
    shared_gate,
    shared_up,
    shared_down,
    expert_ids,
    route_weights,
    expert_gate,
    expert_up,
    expert_down,
):
    block_rows, query_width = queries.shape
    ways = lax.axis_size("tp")
    splits = lax.axis_size("sp")
    width_index = lax.axis_index("tp")
    sp_index = lax.axis_index("sp")
    model_width = out_weight.shape[1]
    own = block_rows // ways
    halves = ways // 2
    experts_here = expert_gate.shape[0]
    experts_all = experts_here * splits
    capacity = max(2, 2 * own * TOPK // experts_all)
    slots = splits * capacity
    turning = splits <= 8
    half = splits // 2

    def over(x, mask):
        return lax.ppermute(x, "tp", [(i, i ^ mask) for i in range(ways)])

    def exchange(x):
        return lax.all_to_all(x, "sp", 0, 0, tiled=True)

    def turned(pieces, masks):
        done = []
        for piece, m in zip(pieces, masks):
            pairs = [(i, i ^ m) for i in range(splits)]
            done.append(lax.ppermute(piece, "sp", pairs) if m else piece)
        return done

    def plus(a, b):
        return (a.astype(F32) + b.astype(F32)).astype(BF)

    def returned(keep, send):
        if not turning:
            keep, send = jnp.concatenate(keep, axis=0), jnp.concatenate(send, axis=0)
            return [exchange(plus(keep, over(send, 2)))]
        pieces = []
        for part in (1, 0):
            other = over(send[part], 2)
            if part == 0:
                other, summed = lax.optimization_barrier((other, summed))
            summed = plus(keep[part], other)
            masks = range(part * half, (part + 1) * half)
            sent = [summed[k * capacity : (k + 1) * capacity] for k in range(half)]
            pieces = turned(sent, masks) + pieces
        return pieces

    up = [(i, i + 1) for i in range(splits - 1)]
    down = [(i + 1, i) for i in range(splits - 1)]
    keys_t, values_t = keys.T, values.T
    tail = jnp.concatenate([keys_t[:, -WINDOW:], values_t[:, -WINDOW:]], axis=0)
    head = jnp.concatenate([keys_t[:, :WINDOW], values_t[:, :WINDOW]], axis=0)
    tp = width_index.reshape(1)
    gain = norm_gain.reshape(1, model_width)
    ids_t = expert_ids.T
    experts = (experts_all, experts_here)
    place = np.arange(slots, dtype=np.int32) // capacity
    rank = (np.arange(slots) % capacity).astype(np.float32)
    turn = (sp_index if turning else sp_index * 0).reshape(1)
    before = lax.ppermute(tail, "sp", up)
    after = lax.ppermute(head, "sp", down)
    quarter = HEAD_DIM // 4
    spectrum = ROPE_BASE ** (-np.arange(quarter, dtype=np.float64) / quarter)
    spectrum = np.concatenate([spectrum, spectrum])[:, None].astype(np.float32)
    attended = call(
        functools.partial(attention_body, total_rows=splits * block_rows),
        [((own, query_width), BF)] * ways + [((block_rows - own, query_width), BF)] * ways,
        (queries.T, keys_t, values_t, before, after, jnp.asarray(spectrum)),
        scalars=(tp, sp_index.reshape(1), sinks),
        scratch=[
            pltpu.VMEM((block_rows, query_width), BF),
            pltpu.VMEM((block_rows + 2 * WINDOW, HEAD_DIM), BF),
            pltpu.VMEM((HEAD_DIM, block_rows + 2 * WINDOW), BF),
        ],
        flops=12 * block_rows * WINDOW * query_width,
        moved=4 * block_rows * query_width,
    )

    combine_weights = call(
        functools.partial(prepare_body, experts=experts),
        [((2, own, slots), BF)] * experts_here,
        (
            ids_t,
            route_weights.T,
            jnp.asarray(place[None, :]),
            jnp.asarray(rank[None, :]),
        ),
        scalars=(tp, turn),
        flops=8 * own * experts_all * slots,
        moved=8 * own * slots,
    )
    out_weight, residual = load((out_weight, residual), (turn,), tp, ways)
    parts = [over(attended[m], m) if m else attended[m] for m in range(ways)]
    rests = [over(attended[ways + m], m) if m else attended[ways + m] for m in range(ways)]
    mixed, *outgoing = call(
        functools.partial(dispatch_body, ways, experts=experts),
        [((own, model_width), BF)] + [((capacity, model_width), BF)] * splits,
        (
            *parts,
            residual,
            out_weight,
            gain,
            ids_t,
            jnp.asarray(place[:, None]),
            jnp.asarray(rank[:, None]),
        ),
        scalars=(tp, turn),
        flops=2 * own * model_width * (out_weight.shape[0] + slots),
        moved=2 * out_weight.size,
    )
    if turning:
        arrived = turned(outgoing, range(splits))
        near = []
        for part in range(2):
            near += joined(arrived[part * half : (part + 1) * half])
    else:
        near = exchange(jnp.concatenate(outgoing, axis=0))
        near = [near[: half * capacity], near[half * capacity :]]
    gain_late = marker(gain)
    combine_weights = [marker(x) for x in combine_weights]

    outgoing = call(
        functools.partial(second_body, ways, experts=experts),
        [((halves * capacity, model_width), BF)] * (splits * (experts_here - 1)),
        (
            *parts,
            *rests,
            residual,
            out_weight,
            gain,
            ids_t,
            jnp.asarray(place[:, None]),
            jnp.asarray(rank[:, None]),
        ),
        scalars=(tp, turn),
        flops=2 * halves * own * model_width * (out_weight.shape[0] + slots),
        moved=2 * out_weight.size,
    )
    sources = (shared_gate, shared_up, shared_down, expert_gate, expert_up, expert_down)
    shared_gate, shared_up, shared_down, *weights = load(sources, (gain_late,), tp, 1)
    keep, send = call(
        functools.partial(shared_body, ways),
        [((halves, own, model_width), BF)] * 2,
        (
            *parts,
            *rests,
            residual,
            out_weight,
            gain_late,
            shared_gate,
            shared_up,
            shared_down,
        ),
        flops=2 * block_rows * model_width * (out_weight.shape[0] + 3 * shared_gate.shape[1]),
        moved=2 * out_weight.size,
    )
    got = over(send, 1)
    shared_own = plus(keep[0], got[0])
    shared_far = over(plus(keep[1], got[1]), 2)

    far_sums, pairs = [None] * 2, [None] * 2
    for part in (1, 0):
        far = over(near[part], 2)
        pairs[part] = over(near[part], 1)
        far_pair = over(far, 1)
        out_pair, out_far = expert_rows(0, [far_pair, far], *weights)
        out_pair = over(out_pair, 1)
        far_sums[part] = plus(out_far, out_pair)
    outs = expert_rows(0, [*pairs, *near], *weights)
    near_sums = [plus(outs[2 + p], over(outs[p], 1)) for p in range(2)]
    back = [returned(near_sums, far_sums)]

    for c in range(1, experts_here):
        pieces = outgoing[splits * (c - 1) : splits * c]
        if turning:
            arrived = turned(pieces, range(splits))
            mine, far = joined(arrived, halves)
        else:
            arrived = exchange(jnp.concatenate(pieces, axis=0))
            arrived = arrived.reshape(splits, halves, capacity, model_width)
            mine, far = (arrived[:, h].reshape(slots, model_width) for h in range(halves))
        far_pair = over(far, 1)
        out_pair, out_far = expert_rows(c, [far_pair, far], *weights)
        far_sum = plus(out_far, over(out_pair, 1))
        pair = over(mine, 1)
        out_pair, out_mine = expert_rows(c, [pair, mine], *weights)
        summed = plus(out_mine, over(out_pair, 1))
        cut = half * capacity
        summed, far_sum = ([x[:cut], x[cut:]] for x in (summed, far_sum))
        back.append(returned(summed, far_sum))

    total = None
    for c in range(experts_here):
        last = c == experts_here - 1
        added = (mixed, shared_own, shared_far) if total is None else (total,)
        total = call(
            functools.partial(combine_body, len(back[c])),
            [((own, model_width), BF if last else F32)],
            (combine_weights[c], *back[c], *added),
            scratch=[pltpu.VMEM((slots, model_width), BF)],
            final=last,
            flops=4 * own * slots * model_width,
            moved=2 * slots * model_width,
        )[0]
    return total


def solution(mesh):
    placed = (
        P("sp", "tp"),
        P("sp", "tp"),
        P("sp", "tp"),
        P("tp"),
        P("sp", None),
        P(),
        P(),
        P(None, "tp"),
        P(None, "tp"),
        P("tp", None),
        P("sp", None),
        P(("sp", "tp"), None),
        P("sp", None, "tp"),
        P("sp", None, "tp"),
        P("sp", "tp", None),
    )
    return jax.shard_map(
        layer, mesh=mesh, in_specs=placed, out_specs=P(("sp", "tp"), None), check_vma=False
    )
```
